32 devices in a mesh: grp: 2 (over x), ep: 8 (over z, y), tp: 2 (over core).
Axes of the slice: x: 2, y: 2, z: 4, core: 2. Of those that a mesh axis runs over, the one named last changes fastest.
Arguments:
- tokens: bfloat16 [8192, 2048], P(('grp', 'ep', 'tp')), parts along dimension 0, may hold values from -6 to 6
- norm_gain: float32 [2048], replicated, may hold values from 0.1 to 1.9
- route_ids: int32 [8192, 2], P(('grp', 'ep', 'tp')), parts along dimension 0, may hold values from 0 to 7, as said below
- route_weights: float32 [8192, 2], P(('grp', 'ep', 'tp')), parts along dimension 0, may hold values from 0.1 to 1
- w_gate: bfloat16 [8, 2048, 512], P('ep', None, 'tp'), may hold values from -0.125 to 0.125
- w_up: bfloat16 [8, 2048, 512], P('ep', None, 'tp'), may hold values from -0.125 to 0.125
- w_down: bfloat16 [8, 512, 2048], P('ep', 'tp'), may hold values from -0.25 to 0.25
Outputs:
- mixed: bfloat16 [8192, 2048], P(('grp', 'ep', 'tp')), parts along dimension 0
The draws below stay inside these ranges and needn't reach their ends.
There are 2 independent parts, one for each index of `grp`. The reference program is written for one: setup_inputs(seed, part) draws one part's arguments, and reference() takes and returns one part's arrays. A program takes and returns all parts, laid end to end along the dimension named above; an argument that names none is the same for every part. Nothing has to cross between parts.
Inputs may be any that keep to these rules, and one draw needn't show every extreme that they name: `route_ids`: the 2 experts of a token are different and lie in one group of 2 consecutive experts. Among the tokens of one device (aligned blocks of 256 tokens) no expert is named more than 128 times, and in every such block some expert is named exactly 128 times.
All inputs are finite; a program needn't handle non-finite values.
Results may differ from the reference program's by a relative error of at most 0.007.
Values may be sent and summed in bfloat16 or wider, within the bound.
No kernel may reach another device: no remote copies, remote signals or barrier semaphores. Data moves between devices by JAX's collectives and lax.ppermute only.
A program may use at most 128 MiB of HBM per device.

```python
import math
import jax
import jax.numpy as jnp
from jax import lax

D = 2048
FF = 512
GROUPS = 4
TOPK = 2
TOK_DEV = 256
EXPERTS = 8
EXP_GROUP = 2
CAP = 128
TOKENS = 4096


def route_block(block_key):
    subkeys = jax.random.split(block_key, 5)
    halfway = TOK_DEV // 2
    busiest = jax.random.randint(subkeys[0], (), 0, GROUPS)
    spare = halfway - (GROUPS - 1) * EXP_GROUP
    cut_points = jnp.sort(jax.random.randint(subkeys[1], (GROUPS - 2,), 0, spare + 1))
    bounds = jnp.concatenate([jnp.zeros((1,), jnp.int32), cut_points.astype(jnp.int32), jnp.full((1,), spare, jnp.int32)])
    group_sizes = jnp.concatenate([jnp.full((1,), halfway, jnp.int32), bounds[1:] - bounds[:-1] + EXP_GROUP])
    bound_ends = jnp.cumsum(group_sizes)
    starts = bound_ends - group_sizes
    position = jnp.arange(TOK_DEV, dtype=jnp.int32)
    group_rank = jnp.sum((position[:, None] >= bound_ends[None, :]).astype(jnp.int32), axis=1)
    within = position - starts[group_rank]
    group = (busiest + group_rank) % GROUPS
    offsets = jax.random.randint(subkeys[2], (GROUPS,), 0, EXP_GROUP)
    shifts = jax.random.randint(subkeys[3], (GROUPS,), 1, EXP_GROUP)
    first_pick = (within + offsets[group]) % EXP_GROUP
    second_pick = (first_pick + shifts[group]) % EXP_GROUP
    chosen = group[:, None] * EXP_GROUP + jnp.stack([first_pick, second_pick], axis=1)
    shuffle = jax.random.permutation(subkeys[4], TOK_DEV)
    return jnp.zeros((TOK_DEV, 2), jnp.int32).at[shuffle].set(chosen.astype(jnp.int32))


def draw_route_ids(key, part):
    block_keys = jax.random.split(jax.random.fold_in(key, 17), TOKENS // TOK_DEV)
    return jax.vmap(route_block)(block_keys).reshape(TOKENS, TOPK).astype(jnp.int32)


def levels(rng, dims, pieces, smallest, high):
    gain, own = 1.0, jax.random.fold_in(rng, 6)
    for dim, shards_of in pieces:
        steps = jnp.exp(jax.random.uniform(jax.random.fold_in(own, dim), (shards_of,), jnp.float32, smallest / len(pieces), high / len(pieces)))
        gain = gain * jnp.repeat(steps, dims[dim] // shards_of).reshape([-1 if axis == dim else 1 for axis in range(len(dims))])
    return gain


def gaussian(rng, dims, width, reach, pieces=(), held_as=jnp.bfloat16):
    loudness = levels(rng, dims, pieces, -0.22, 0.18) if pieces else 1.0
    result = jax.random.normal(rng, dims, jnp.float32) * width * loudness
    return jnp.minimum(jnp.maximum(result, -reach), reach).astype(held_as)


def setup_inputs(seed: int = 0, part: int = 0) -> dict:
    streams_of = jax.random.split(jax.random.key(seed), 8)
    own_keys = jax.random.split(jax.random.fold_in(streams_of[7], part), 8)
    return {
        "tokens": gaussian(own_keys[0], (TOKENS, D), 1.0, 6.0, ((0, 16),)),
        "norm_gain": jnp.clip(1.0 + 0.18 * jax.random.normal(streams_of[1], (D,), jnp.float32), 0.1, 1.9),
        "route_ids": draw_route_ids(jax.random.fold_in(jax.random.fold_in(streams_of[7], part), 71), part),
        "route_weights": jnp.clip(jnp.exp(math.log(1.0) - 2.3025851 * jax.random.uniform(own_keys[3], (TOKENS, TOPK), jnp.float32) ** levels(own_keys[3], (TOKENS, TOPK), ((0, 16),), -0.2, 0.2)), 0.1, 1.0),
        "w_gate": gaussian(streams_of[4], (EXPERTS, D, FF), D ** -0.5, 0.125, ((0, 8), (2, 2))),
        "w_up": gaussian(streams_of[5], (EXPERTS, D, FF), D ** -0.5, 0.125, ((0, 8), (2, 2))),
        "w_down": gaussian(streams_of[6], (EXPERTS, FF, D), FF ** -0.5, 0.25, ((0, 8), (1, 2))),
    }


epsilon = 1e-06

def reference(tokens, norm_gain, route_ids, route_weights, w_gate, w_up, w_down):
    floats = tokens.astype(jnp.float32)
    inverse = lax.rsqrt(lax.optimization_barrier(jnp.mean(floats * floats, axis=1, keepdims=True)) + epsilon)
    normed = (floats * inverse * norm_gain.astype(jnp.float32)).astype(jnp.bfloat16)
    blocks = TOKENS // TOK_DEV
    route_flat = route_ids.reshape(blocks, TOK_DEV * TOPK).astype(jnp.int32)
    onehot = (route_flat[:, :, None] == jnp.arange(EXPERTS, dtype=jnp.int32)[None, None, :]).astype(jnp.int32)
    slot_index = lax.optimization_barrier(jnp.sum((jnp.cumsum(onehot, axis=1) - onehot) * onehot, axis=2)).astype(jnp.int32)
    anchor = jnp.arange(blocks, dtype=jnp.int32)[:, None]
    position = ((route_flat * blocks + anchor) * CAP + slot_index).astype(jnp.int32)
    position = position.reshape(TOKENS, TOPK)
    buffer = jnp.zeros((EXPERTS * blocks * CAP, D), jnp.bfloat16)
    for column in range(TOPK):
        buffer = buffer.at[position[:, column]].set(normed)
    buffer = buffer.reshape(EXPERTS, blocks * CAP, D)

    def expert(inputs):
        batch_rows, gate_weight, up_weight, down_weight = inputs
        gate_pre = jnp.dot(batch_rows, gate_weight, preferred_element_type=jnp.float32)
        up_pre = jnp.dot(batch_rows, up_weight, preferred_element_type=jnp.float32)
        hidden = (jax.nn.silu(gate_pre) * up_pre).astype(jnp.bfloat16)
        return jnp.dot(hidden, down_weight, preferred_element_type=jnp.float32).astype(jnp.bfloat16)
    results = lax.map(expert, (buffer, w_gate, w_up, w_down)).reshape(EXPERTS * blocks * CAP, D)
    combined = jnp.zeros((TOKENS, D), jnp.float32)
    for column in range(TOPK):
        picked = results[position[:, column]].astype(jnp.float32)
        combined = combined + route_weights[:, column:column + 1].astype(jnp.float32) * picked
    return combined.astype(jnp.bfloat16)
```

```python
import jax
import jax.numpy as jnp
from jax import lax
from jax.sharding import PartitionSpec as P

GROUPS = 4

epsilon = 1e-06


def normalize(tokens, norm_gain):
    floats = tokens.astype(jnp.float32)
    inverse = lax.rsqrt(jnp.mean(floats * floats, axis=1, keepdims=True) + epsilon)
    return (floats * inverse * norm_gain).astype(jnp.bfloat16)


def routed_by_expert(tokens, norm_gain, route_ids, route_weights, w_gate, w_up, w_down):
    row_count, features = tokens.shape
    top_count = route_ids.shape[1]
    local_experts = w_gate.shape[0]
    ep_size = lax.axis_size("ep")
    experts_all = ep_size * local_experts
    capacity = row_count * GROUPS // experts_all
    normed = normalize(tokens, norm_gain)
    flat_ids = route_ids.reshape(-1)
    onehot = (flat_ids[:, None] == jnp.arange(experts_all, dtype=jnp.int32)[None, :]).astype(
        jnp.int32
    )
    earlier = jnp.cumsum(onehot, axis=0) - onehot
    slot_index = jnp.sum(earlier * onehot, axis=1)
    target = (flat_ids * capacity + slot_index).reshape(row_count, top_count)
    outbound = jnp.zeros((experts_all * capacity, features), jnp.bfloat16)
    for column in range(top_count):
        outbound = outbound.at[target[:, column]].set(normed)
    outbound = outbound.reshape(ep_size, local_experts, capacity, features)
    full_gate, full_up, full_down = (
        lax.all_gather(w_gate, "tp", axis=2, tiled=True),
        lax.all_gather(w_up, "tp", axis=2, tiled=True),
        lax.all_gather(w_down, "tp", axis=1, tiled=True),
    )
    arrived = lax.all_to_all(outbound, "ep", split_axis=0, concat_axis=0, tiled=True)
    gate_pre = jnp.einsum("sjcd,jdf->sjcf", arrived, full_gate, preferred_element_type=jnp.float32)
    up_pre = jnp.einsum("sjcd,jdf->sjcf", arrived, full_up, preferred_element_type=jnp.float32)
    hidden = (jax.nn.silu(gate_pre) * up_pre).astype(jnp.bfloat16)
    result = jnp.einsum("sjcf,jfd->sjcd", hidden, full_down, preferred_element_type=jnp.float32)
    returned_rows = lax.all_to_all(
        result.astype(jnp.bfloat16), "ep", split_axis=0, concat_axis=0, tiled=True
    )
    returned_rows = returned_rows.reshape(experts_all * capacity, features)
    combined = jnp.zeros((row_count, features), jnp.float32)
    for column in range(top_count):
        picked = returned_rows[target[:, column]].astype(jnp.float32)
        combined = combined + route_weights[:, column : column + 1] * picked
    return combined.astype(jnp.bfloat16)


def routed_by_group(tokens, norm_gain, route_ids, route_weights, w_gate, w_up, w_down):
    row_count, features = tokens.shape
    members = route_ids.shape[1]
    ep_size = lax.axis_size("ep")
    capacity = row_count * GROUPS // ep_size
    me = lax.axis_index("ep")
    my_group, my_member = me // members, me % members

    def hop(value, distance):
        pairs = [
            (i, ((i // members) ^ distance) * members + i % members) for i in range(ep_size)
        ]
        return lax.ppermute(value, "ep", pairs)

    normed = normalize(tokens, norm_gain)
    ids = route_ids.T
    distance_of = (ids[0] // members) ^ my_group
    onehot = (distance_of[None, :] == jnp.arange(GROUPS, dtype=jnp.int32)[:, None])
    triangle = (
        jnp.arange(row_count)[:, None] <= jnp.arange(row_count)[None, :]
    ).astype(jnp.bfloat16)
    ranks = jnp.dot(onehot.astype(jnp.bfloat16), triangle, preferred_element_type=jnp.float32)
    rank = jnp.sum(jnp.where(onehot, ranks, 0.0), axis=0).astype(jnp.int32) - 1
    target = distance_of * capacity + rank
    place = target[None, :] == jnp.arange(GROUPS * capacity, dtype=jnp.int32)[:, None]
    selector = place.astype(jnp.bfloat16)
    outbound = jnp.dot(selector, normed, preferred_element_type=jnp.float32).astype(jnp.bfloat16)
    outbound = outbound.reshape(GROUPS, capacity, features)
    by_member = [
        jnp.sum(jnp.where(ids % members == m, route_weights.T, 0.0), axis=0)
        for m in range(members)
    ]
    slot_weights = jnp.stack(
        [jnp.sum(jnp.where(place, w[None, :], 0.0), axis=1) for w in by_member]
    ).reshape(members, GROUPS, capacity)

    arrived = [outbound[0]] + [None] * (GROUPS - 1)
    weights = [slot_weights[:, 0]] + [None] * (GROUPS - 1)
    for distance in range(GROUPS - 1, 0, -1):
        arrived[distance] = hop(outbound[distance], distance)
        weights[distance] = hop(slot_weights[:, distance], distance)
    rows = jnp.concatenate(arrived, axis=0)
    row_weights = jnp.concatenate(weights, axis=1)

    def beside(value):
        return lax.ppermute(value, "tp", [(0, 1), (1, 0)])

    experts = []
    quarter = (w_gate[0], w_up[0], w_down[0])
    for step in range(members):
        if step:
            pairs = [
                (i, (i // members) * members + (i + 1) % members) for i in range(ep_size)
            ]
            quarter = tuple(lax.ppermute(w, "ep", pairs) for w in quarter)
        experts.append((quarter, tuple(beside(w) for w in quarter)))
    mixed = jnp.zeros((GROUPS * capacity, features), jnp.float32)
    for step, halves in enumerate(experts):
        total = 0.0
        for gate_w, up_w, down_w in halves:
            gate_pre = jnp.dot(rows, gate_w, preferred_element_type=jnp.float32)
            up_pre = jnp.dot(rows, up_w, preferred_element_type=jnp.float32)
            hidden = (jax.nn.silu(gate_pre) * up_pre).astype(jnp.bfloat16)
            total = total + jnp.dot(hidden, down_w, preferred_element_type=jnp.float32)
        member = (my_member + members - step) % members
        scale = lax.dynamic_index_in_dim(row_weights, member, 0, keepdims=False)
        mixed = mixed + scale[:, None] * total.astype(jnp.bfloat16).astype(jnp.float32)
    mixed = mixed.astype(jnp.bfloat16).reshape(GROUPS, capacity, features)
    back = [mixed[0]] + [None] * (GROUPS - 1)
    for distance in range(GROUPS - 1, 0, -1):
        back[distance] = hop(mixed[distance], distance)
    back = jnp.concatenate(back, axis=0)
    return jnp.dot(selector.T, back, preferred_element_type=jnp.float32).astype(jnp.bfloat16)


def per_device(tokens, norm_gain, route_ids, route_weights, w_gate, w_up, w_down):
    local_experts = w_gate.shape[0]
    members = lax.axis_size("ep") * local_experts // GROUPS
    if local_experts == 1 and members == route_ids.shape[1]:
        step = routed_by_group
    else:
        step = routed_by_expert
    return step(tokens, norm_gain, route_ids, route_weights, w_gate, w_up, w_down)


def solution(mesh):
    in_specs = (
        P(("grp", "ep", "tp"), None),
        P(),
        P(("grp", "ep", "tp"), None),
        P(("grp", "ep", "tp"), None),
        P("ep", None, "tp"),
        P("ep", None, "tp"),
        P("ep", "tp", None),
    )
    out_specs = P(("grp", "ep", "tp"), None)
    return jax.shard_map(
        per_device, mesh=mesh, in_specs=in_specs, out_specs=out_specs, check_vma=False
    )
```

```python
import functools

import jax
import jax.numpy as jnp
from jax import lax
from jax.experimental import pallas as pl
from jax.experimental.pallas import tpu as pltpu
from jax.sharding import PartitionSpec as P

GROUPS = 4

epsilon = 1e-06


def normalize(tokens, norm_gain):
    floats = tokens.astype(jnp.float32)
    inverse = lax.rsqrt(jnp.mean(floats * floats, axis=1, keepdims=True) + epsilon)
    return (floats * inverse * norm_gain).astype(jnp.bfloat16)


def routed_by_expert(tokens, norm_gain, route_ids, route_weights, w_gate, w_up, w_down):
    row_count, features = tokens.shape
    top_count = route_ids.shape[1]
    local_experts = w_gate.shape[0]
    ep_size = lax.axis_size("ep")
    experts_all = ep_size * local_experts
    capacity = row_count * GROUPS // experts_all
    normed = normalize(tokens, norm_gain)
    flat_ids = route_ids.reshape(-1)
    onehot = (flat_ids[:, None] == jnp.arange(experts_all, dtype=jnp.int32)[None, :]).astype(
        jnp.int32
    )
    earlier = jnp.cumsum(onehot, axis=0) - onehot
    slot_index = jnp.sum(earlier * onehot, axis=1)
    target = (flat_ids * capacity + slot_index).reshape(row_count, top_count)
    outbound = jnp.zeros((experts_all * capacity, features), jnp.bfloat16)
    for column in range(top_count):
        outbound = outbound.at[target[:, column]].set(normed)
    outbound = outbound.reshape(ep_size, local_experts, capacity, features)
    full_gate, full_up, full_down = (
        lax.all_gather(w_gate, "tp", axis=2, tiled=True),
        lax.all_gather(w_up, "tp", axis=2, tiled=True),
        lax.all_gather(w_down, "tp", axis=1, tiled=True),
    )
    arrived = lax.all_to_all(outbound, "ep", split_axis=0, concat_axis=0, tiled=True)
    gate_pre = jnp.einsum("sjcd,jdf->sjcf", arrived, full_gate, preferred_element_type=jnp.float32)
    up_pre = jnp.einsum("sjcd,jdf->sjcf", arrived, full_up, preferred_element_type=jnp.float32)
    hidden = (jax.nn.silu(gate_pre) * up_pre).astype(jnp.bfloat16)
    result = jnp.einsum("sjcf,jfd->sjcd", hidden, full_down, preferred_element_type=jnp.float32)
    returned_rows = lax.all_to_all(
        result.astype(jnp.bfloat16), "ep", split_axis=0, concat_axis=0, tiled=True
    )
    returned_rows = returned_rows.reshape(experts_all * capacity, features)
    combined = jnp.zeros((row_count, features), jnp.float32)
    for column in range(top_count):
        picked = returned_rows[target[:, column]].astype(jnp.float32)
        combined = combined + route_weights[:, column : column + 1] * picked
    return combined.astype(jnp.bfloat16)


def narrow_sum(mask, values, axis):
    return jnp.sum(jnp.where(mask, values, 0), axis=axis, keepdims=True)


def diagonal(size):
    return lax.broadcasted_iota(jnp.int32, (size, size), 0) == lax.broadcasted_iota(
        jnp.int32, (size, size), 1
    )


def pack_kernel(members, capacity, tokens, gain, ids, weights, target_out, *outs):
    packed, scales = outs[:GROUPS], outs[GROUPS:]
    row_count = tokens.shape[0]
    my_group = lax.axis_index("ep") // members
    first = ids[0:1, :]
    group = jnp.zeros_like(first)
    for bound in range(1, GROUPS):
        group += (first >= bound * members).astype(jnp.int32)
    distance = group ^ my_group
    onehot = lax.broadcasted_iota(jnp.int32, (16, row_count), 0) == distance
    triangle = lax.broadcasted_iota(
        jnp.int32, (row_count, row_count), 0
    ) <= lax.broadcasted_iota(jnp.int32, (row_count, row_count), 1)
    ranks = jnp.dot(
        onehot.astype(jnp.float32).astype(jnp.bfloat16),
        triangle.astype(jnp.float32).astype(jnp.bfloat16),
        preferred_element_type=jnp.float32,
    )
    rank = narrow_sum(onehot, ranks, 0).astype(jnp.int32) - 1
    target = distance * capacity + rank
    target_out[...] = target
    floats = tokens[...].astype(jnp.float32)
    inverse = lax.rsqrt(jnp.mean(floats * floats, axis=1, keepdims=True) + epsilon)
    normed = (floats * inverse * gain[...]).astype(jnp.bfloat16)
    eye = diagonal(capacity)
    for step in range(GROUPS - 1, -1, -1):
        place = (
            lax.broadcasted_iota(jnp.int32, (capacity, row_count), 0) + step * capacity
            == target
        )
        packed[step][...] = jnp.dot(
            place.astype(jnp.float32).astype(jnp.bfloat16),
            normed,
            preferred_element_type=jnp.float32,
        ).astype(jnp.bfloat16)
        for member in range(members):
            by_token = jnp.zeros((1, row_count), jnp.float32)
            for column in range(ids.shape[0]):
                named = ids[column : column + 1, :] - group * members == member
                by_token += jnp.where(named, weights[column : column + 1, :], 0.0)
            by_slot = narrow_sum(place, by_token, 1)
            scales[step][member : member + 1, :] = narrow_sum(eye, by_slot, 0)


def pack(tokens, norm_gain, ids, weights, members, capacity):
    row_count, features = tokens.shape
    outs = pl.pallas_call(
        functools.partial(pack_kernel, members, capacity),
        out_shape=[jax.ShapeDtypeStruct((1, row_count), jnp.int32)]
        + [jax.ShapeDtypeStruct((capacity, features), jnp.bfloat16)] * GROUPS
        + [jax.ShapeDtypeStruct((members, capacity), jnp.float32)] * GROUPS,
        cost_estimate=pl.CostEstimate(
            flops=2 * GROUPS * capacity * row_count * features,
            bytes_accessed=6 * row_count * features,
            transcendentals=0,
        ),
        compiler_params=pltpu.CompilerParams(vmem_limit_bytes=24 << 20),
        name="pack",
    )(tokens, norm_gain[None, :], ids, weights)
    return outs[0], outs[1 : 1 + GROUPS], outs[1 + GROUPS :]


def unpack_kernel(capacity, target, *refs):
    pieces, out = refs[:-1], refs[-1]
    row_count = out.shape[0]
    column = narrow_sum(diagonal(row_count), target[...], 1)
    total = jnp.zeros(out.shape, jnp.float32)
    for step, piece in enumerate(pieces):
        place = (
            lax.broadcasted_iota(jnp.int32, (row_count, capacity), 1) + step * capacity
            == column
        )
        total += jnp.dot(
            place.astype(jnp.float32).astype(jnp.bfloat16),
            piece[...],
            preferred_element_type=jnp.float32,
        )
    out[...] = total.astype(jnp.bfloat16)


def unpack(target, pieces):
    row_count = target.shape[1]
    capacity, features = pieces[0].shape
    tile = features // 4
    return pl.pallas_call(
        functools.partial(unpack_kernel, capacity),
        grid=(4,),
        in_specs=[pl.BlockSpec((1, row_count), lambda i: (0, 0))]
        + [pl.BlockSpec((capacity, tile), lambda i: (0, i))] * len(pieces),
        out_specs=pl.BlockSpec((row_count, tile), lambda i: (0, i)),
        out_shape=jax.ShapeDtypeStruct((row_count, features), jnp.bfloat16),
        cost_estimate=pl.CostEstimate(
            flops=2 * len(pieces) * capacity * row_count * features,
            bytes_accessed=6 * row_count * features,
            transcendentals=0,
        ),
        compiler_params=pltpu.CompilerParams(vmem_limit_bytes=16 << 20),
        name="unpack",
    )(target, *pieces)


def expert_kernel(count, quarters, *refs):
    rows, scales = refs[:count], refs[count : 2 * count]
    sources = refs[2 * count : -(9 + count)]
    outs = refs[-(9 + count) : -9]
    x, gate, up, down, hidden, mixed, sem_x, sem_w, sem_out = refs[-9:]
    capacity, features = rows[0].shape
    part = lax.axis_index("grp")
    member = lax.axis_index("ep") % 2
    row_copies = [
        pltpu.make_async_copy(ref, x.at[pl.ds(i * capacity, capacity)], sem_x.at[i])
        for i, ref in enumerate(rows)
    ]
    for copy in row_copies:
        copy.start()
    for kind, stack in enumerate((gate, up, down)):
        for q, quarter in enumerate(quarters):
            for choice in range(2):
                if quarter[kind][0] == quarter[kind][1] and choice:
                    continue
                copy = pltpu.make_async_copy(
                    sources[quarter[kind][choice]], stack.at[q], sem_w.at[kind, q]
                )
                if quarter[kind][0] == quarter[kind][1]:
                    copy.start()
                else:
                    pl.when(part == choice)(copy.start)
    for copy in row_copies:
        copy.wait()

    def arrived(kind, q):
        stack = (gate, up, down)[kind]
        pltpu.make_async_copy(stack.at[q], stack.at[q], sem_w.at[kind, q]).wait()

    @pl.loop(0, len(quarters))
    def _(q):
        arrived(0, q)
        gate_pre = jnp.dot(x[...], gate[q], preferred_element_type=jnp.float32)
        arrived(1, q)
        up_pre = jnp.dot(x[...], up[q], preferred_element_type=jnp.float32)
        hidden[q] = (gate_pre / (1.0 + jnp.exp(-gate_pre)) * up_pre).astype(jnp.bfloat16)

    eye = diagonal(capacity)
    columns = []
    for which in range(2):
        row = lax.rem(member + which, 2)
        columns.append(
            jnp.concatenate(
                [narrow_sum(eye, s[pl.ds(row, 1), :], 1) for s in scales], axis=0
            )
        )
    for q in range(len(quarters)):
        arrived(2, q)
    tile = 512

    @pl.loop(0, features // tile)
    def _(n):
        lanes = pl.ds(pl.multiple_of(n * tile, tile), tile)
        total = 0.0
        for which in range(2):
            result = 0.0
            for q in (2 * which, 2 * which + 1):
                result = result + jnp.dot(
                    hidden[q], down[q, :, lanes], preferred_element_type=jnp.float32
                )
            total = total + columns[which] * result.astype(jnp.bfloat16).astype(jnp.float32)
        mixed[:, lanes] = total.astype(jnp.bfloat16)

    out_copies = [
        pltpu.make_async_copy(mixed.at[pl.ds(i * capacity, capacity)], ref, sem_out.at[i])
        for i, ref in enumerate(outs)
    ]
    for copy in out_copies:
        copy.start()
    for copy in out_copies:
        copy.wait()


def experts(rows, scales, sources, quarters):
    count = len(rows)
    capacity, features = rows[0].shape
    half = sources[0].shape[1]
    total = count * capacity
    anywhere = pl.BlockSpec(memory_space=pl.ANY)
    vmem = pl.BlockSpec(memory_space=pltpu.VMEM)
    return pl.pallas_call(
        functools.partial(expert_kernel, count, quarters),
        out_shape=[jax.ShapeDtypeStruct((capacity, features), jnp.bfloat16)] * count,
        in_specs=[anywhere] * count + [vmem] * count + [anywhere] * len(sources),
        out_specs=[anywhere] * count,
        scratch_shapes=[
            pltpu.VMEM((total, features), jnp.bfloat16),
            pltpu.VMEM((4, features, half), jnp.bfloat16),
            pltpu.VMEM((4, features, half), jnp.bfloat16),
            pltpu.VMEM((4, half, features), jnp.bfloat16),
            pltpu.VMEM((4, total, half), jnp.bfloat16),
            pltpu.VMEM((total, features), jnp.bfloat16),
            pltpu.SemaphoreType.DMA((count,)),
            pltpu.SemaphoreType.DMA((3, 4)),
            pltpu.SemaphoreType.DMA((count,)),
        ],
        cost_estimate=pl.CostEstimate(
            flops=2 * 12 * total * features * half,
            bytes_accessed=24 * features * half + 4 * total * features,
            transcendentals=4 * total * half,
        ),
        compiler_params=pltpu.CompilerParams(vmem_limit_bytes=40 << 20),
        name="experts",
    )(*rows, *scales, *sources)


def routed_by_group(tokens, norm_gain, route_ids, route_weights, w_gate, w_up, w_down):
    row_count, features = tokens.shape
    members = route_ids.shape[1]
    ep_size = lax.axis_size("ep")
    capacity = row_count * GROUPS // ep_size
    axes = ("grp", "ep", "tp")
    cells = [(p, e, c) for p in range(2) for e in range(ep_size) for c in range(2)]
    number = {cell: i for i, cell in enumerate(cells)}

    def send(value, where):
        pairs = [(number[cell], number[where(*cell)]) for cell in cells if where(*cell)]
        return lax.ppermute(value, axes, pairs)

    def hop(value, distance):
        return send(
            value, lambda p, e, c: (p, ((e // members) ^ distance) * members + e % members, c)
        )

    def across(value, only=None):
        return send(
            value, lambda p, e, c: (p, e ^ 1, c) if only in (None, p) else None
        )

    def other_part(value, source):
        return send(value, lambda p, e, c: (1 - p, e, c) if p == source else None)

    def beside(value, only=None):
        return send(value, lambda p, e, c: (p, e, 1 - c) if only in (None, p) else None)

    target, packed, scales = pack(
        tokens, norm_gain, route_ids.T, route_weights.T, members, capacity
    )
    own = (w_gate[0], w_up[0], w_down[0])
    gate_0 = across(own[0], 0)
    up_1 = across(own[1], 1)
    down_n = across(own[2])
    arrived = [packed[0], None, None, None]
    arrived_scales = [scales[0], None, None, None]
    for distance in (3, 2, 1):
        arrived[distance] = hop(packed[distance], distance)
        arrived_scales[distance] = hop(scales[distance], distance)
    partner = tuple(beside(w) for w in own)
    gate_1 = other_part(gate_0, 0)
    up_0 = other_part(up_1, 1)
    partner_gate = (beside(gate_0, 0), beside(gate_1, 1))
    partner_up = (beside(up_0, 0), beside(up_1, 1))
    partner_down = beside(down_n)
    sources = own + partner + (gate_0, gate_1, up_0, up_1, down_n)
    sources += partner_gate + partner_up + (partner_down,)
    quarters = (
        ((0, 0), (1, 1), (2, 2)),
        ((3, 3), (4, 4), (5, 5)),
        ((6, 7), (8, 9), (10, 10)),
        ((11, 12), (13, 14), (15, 15)),
    )
    back = [None] * GROUPS
    for batch in ((3, 2), (1, 0)):
        done = experts(
            [arrived[d] for d in batch], [arrived_scales[d] for d in batch], sources, quarters
        )
        for d, value in zip(batch, done):
            back[d] = hop(value, d) if d else value
    return unpack(target, back)


def per_device(tokens, norm_gain, route_ids, route_weights, w_gate, w_up, w_down):
    members = lax.axis_size("ep") * w_gate.shape[0] // GROUPS
    pairs = w_gate.shape[0] == 1 and members == 2 == route_ids.shape[1]
    if pairs and lax.axis_size("grp") == 2 == lax.axis_size("tp"):
        step = routed_by_group
    else:
        step = routed_by_expert
    return step(tokens, norm_gain, route_ids, route_weights, w_gate, w_up, w_down)


def solution(mesh):
    in_specs = (
        P(("grp", "ep", "tp"), None),
        P(),
        P(("grp", "ep", "tp"), None),
        P(("grp", "ep", "tp"), None),
        P("ep", None, "tp"),
        P("ep", None, "tp"),
        P("ep", "tp", None),
    )
    out_specs = P(("grp", "ep", "tp"), None)
    return jax.shard_map(
        per_device, mesh=mesh, in_specs=in_specs, out_specs=out_specs, check_vma=False
    )
```
